32 devices in a mesh: sp: 8 (over z, x), tp: 4 (over y, core).
Axes of the slice: x: 2, y: 2, z: 4, core: 2. Of those that a mesh axis runs over, the one named last changes fastest.
Arguments:
- tokens: bfloat16 [4096, 2048], P(('sp', 'tp')), may hold values from -8 to 8
- in_gain: float32 [2048], replicated, may hold values from 0.1 to 1.9
- w_conv_val: bfloat16 [2048, 1024], P('sp', 'tp'), may hold values from -0.125 to 0.125
- w_conv_gate: bfloat16 [2048, 1024], P('sp', 'tp'), may hold values from -0.125 to 0.125
- w_query: bfloat16 [2048, 1024], P('sp', 'tp'), may hold values from -1 to 1
- w_key: bfloat16 [2048, 256], P('sp', 'tp'), may hold values from -1 to 1
- value_weight: bfloat16 [2048, 256], P('sp', 'tp'), may hold values from -0.125 to 0.125
- conv_taps: float32 [31, 1024], P(None, 'tp'), may hold values from -1 to 1
- conv_bias: float32 [1024], P('tp'), may hold values from -3 to 3
- norm_gain: float32 [1024], P('tp'), may hold values from 0.1 to 1.9
- norm_bias: float32 [1024], P('tp'), may hold values from -3 to 3
- head_sink_logit: float32 [16], P('tp'), may hold values from 4 to 7
- w_out_conv: bfloat16 [1024, 2048], P('tp', 'sp'), may hold values from -0.125 to 0.125
- w_out_attn: bfloat16 [1024, 2048], P('tp', 'sp'), may hold values from -0.125 to 0.125
Outputs:
- mixed: bfloat16 [4096, 2048], P(('sp', 'tp'))
- log_total: float32 [4096, 16], P('sp', 'tp')
The draws below stay inside these ranges and needn't reach their ends.
All inputs are finite; a program needn't handle non-finite values.
Results may differ from the reference program's by a relative error of at most 0.012.
Values may be sent and summed in bfloat16 or wider, within the bound.
A program may use at most 64 MiB of HBM per device.

```python
import math
import jax
import jax.numpy as jnp
from jax import lax

MODEL_WIDTH = 2048
CONV = 1024
QUERY_HEADS = 16
KEY_VALUE_HEADS = 4
HEAD_WIDTH = 64
CONV_TAPS = 31
WINDOW_REACH = 128
TOK_DEV = 512
TOKENS = 4096


def planted_parts(key):
    random_seed_key = jax.random.fold_in(key, 101)
    direction = jnp.where(jax.random.bernoulli(jax.random.fold_in(random_seed_key, 1), 0.5, (MODEL_WIDTH,)), 1.0, -1.0).astype(jnp.float32)
    mask_pattern = jnp.where(jax.random.bernoulli(jax.random.fold_in(random_seed_key, 2), 0.5, (KEY_VALUE_HEADS, HEAD_WIDTH)), 1.0, -1.0).astype(jnp.float32)
    strength = math.sqrt(288.0) / HEAD_WIDTH ** 0.25
    return (direction, mask_pattern, strength)


def draw_tokens(key, part):
    direction, mask_pattern, strength = planted_parts(key)
    jitter = jnp.clip(jax.random.normal(jax.random.fold_in(key, 201), (TOKENS, MODEL_WIDTH), jnp.float32), -4.0, 4.0)
    levels = jnp.exp(jax.random.uniform(jax.random.fold_in(key, 202), (TOKENS, 1), jnp.float32, math.log(0.7), math.log(4.0)))
    chosen = jax.random.bernoulli(jax.random.fold_in(key, 203), 0.125, (TOKENS, 1))
    result = jnp.where(chosen, levels * direction[None, :] + jitter, jitter)
    return result.astype(jnp.bfloat16)


def draw_w_query(key, part):
    direction, mask_pattern, strength = planted_parts(key)
    random_draws = jnp.clip(jax.random.normal(jax.random.fold_in(key, 301), (MODEL_WIDTH, QUERY_HEADS * HEAD_WIDTH), jnp.float32), -4.0, 4.0) * MODEL_WIDTH ** (-0.5)
    column_list = jnp.repeat(mask_pattern, QUERY_HEADS // KEY_VALUE_HEADS, axis=0).reshape(QUERY_HEADS * HEAD_WIDTH)
    result = random_draws + strength / MODEL_WIDTH * direction[:, None] * column_list[None, :]
    return result.astype(jnp.bfloat16)


def draw_w_key(key, part):
    direction, mask_pattern, strength = planted_parts(key)
    random_draws = jnp.clip(jax.random.normal(jax.random.fold_in(key, 401), (MODEL_WIDTH, KEY_VALUE_HEADS * HEAD_WIDTH), jnp.float32), -4.0, 4.0) * MODEL_WIDTH ** (-0.5)
    column_list = mask_pattern.reshape(KEY_VALUE_HEADS * HEAD_WIDTH)
    result = random_draws + strength / MODEL_WIDTH * direction[:, None] * column_list[None, :]
    return result.astype(jnp.bfloat16)


def shard_levels(own_key, dims, split, smallest, high):
    def one(dim, parts):
        steps = jax.random.uniform(jax.random.fold_in(jax.random.fold_in(own_key, 6), dim), (parts,), jnp.float32, smallest / len(split), high / len(split))
        return jnp.repeat(jnp.exp(steps), dims[dim] // parts).reshape((-1,) + (1,) * (len(dims) - dim - 1))

    factor_of = one(*split[0])
    for cut in split[1:]:
        factor_of = factor_of * one(*cut)
    return factor_of


def centred(key, extent, scale, most, shards=(), held_as=jnp.bfloat16):
    entries = scale * jax.random.normal(key, extent, jnp.float32)
    if shards:
        entries = entries * shard_levels(key, extent, shards, -0.22, 0.18)
    return jnp.clip(entries, -most, most).astype(held_as)


def setup_inputs(seed: int = 0) -> dict:
    splits = jax.random.split(jax.random.key(seed), 15)
    return {
        "tokens": draw_tokens(jax.random.fold_in(splits[14], 71), 0),
        "in_gain": jnp.clip(1.0 + 0.18 * jax.random.normal(splits[1], (MODEL_WIDTH,), jnp.float32), 0.1, 1.9),
        "w_conv_val": centred(splits[2], (MODEL_WIDTH, CONV), MODEL_WIDTH ** -0.5, 0.125, ((0, 8), (1, 4))),
        "w_conv_gate": centred(splits[3], (MODEL_WIDTH, CONV), MODEL_WIDTH ** -0.5, 0.125, ((0, 8), (1, 4))),
        "w_query": draw_w_query(jax.random.fold_in(splits[14], 71), 0),
        "w_key": draw_w_key(jax.random.fold_in(splits[14], 71), 0),
        "value_weight": centred(splits[6], (MODEL_WIDTH, KEY_VALUE_HEADS * HEAD_WIDTH), MODEL_WIDTH ** -0.5, 0.125, ((0, 8), (1, 4))),
        "conv_taps": centred(splits[7], (CONV_TAPS, CONV), CONV_TAPS ** -0.5, 1.0, ((1, 4),), jnp.float32),
        "conv_bias": centred(splits[8], (CONV,), 0.5, 3.0, ((0, 4),), jnp.float32),
        "norm_gain": jnp.clip(1.0 + 0.18 * jax.random.normal(splits[9], (CONV,), jnp.float32), 0.1, 1.9),
        "norm_bias": centred(splits[10], (CONV,), 0.5, 3.0, ((0, 4),), jnp.float32),
        "head_sink_logit": jnp.clip(4.0 + 3.0 * jax.random.uniform(splits[11], (QUERY_HEADS,), jnp.float32) ** shard_levels(splits[11], (QUERY_HEADS,), ((0, 4),), -0.2, 0.2), 4.0, 7.0),
        "w_out_conv": centred(splits[12], (CONV, MODEL_WIDTH), (CONV + QUERY_HEADS * HEAD_WIDTH) ** -0.5, 0.125, ((0, 4), (1, 8))),
        "w_out_attn": centred(splits[13], (QUERY_HEADS * HEAD_WIDTH, MODEL_WIDTH), (CONV + QUERY_HEADS * HEAD_WIDTH) ** -0.5, 0.125, ((0, 4), (1, 8))),
    }


def reference(tokens, in_gain, w_conv_val, w_conv_gate, w_query, w_key, value_weight, conv_taps, conv_bias, norm_gain, norm_bias, head_sink_logit, w_out_conv, w_out_attn):
    every_row = tokens.shape[0]
    flt = tokens.astype(jnp.float32)
    normed = (flt * lax.rsqrt(lax.optimization_barrier(jnp.mean(flt * flt, axis=-1, keepdims=True)) + 1e-06) * in_gain).astype(jnp.bfloat16)
    val_part = jnp.dot(normed, w_conv_val, preferred_element_type=jnp.float32)
    gate_part = jnp.dot(normed, w_conv_gate, preferred_element_type=jnp.float32)
    glu = (val_part * jax.nn.sigmoid(gate_part)).astype(jnp.bfloat16)
    half = CONV_TAPS // 2
    padded = jnp.pad(glu, ((half, half), (0, 0)))
    filtered = jnp.zeros(glu.shape, jnp.float32) + conv_bias
    for offset in range(CONV_TAPS):
        filtered = filtered + padded[offset:offset + every_row].astype(jnp.float32) * conv_taps[offset]
    center = lax.optimization_barrier(jnp.mean(filtered, axis=-1, keepdims=True))
    spread = lax.optimization_barrier(jnp.mean((filtered - center) ** 2, axis=-1, keepdims=True))
    conv_out = jax.nn.silu((filtered - center) * lax.rsqrt(spread + 1e-05) * norm_gain + norm_bias).astype(jnp.bfloat16)
    query_matrix = jnp.dot(normed, w_query, preferred_element_type=jnp.float32).astype(jnp.bfloat16)
    key = jnp.dot(normed, w_key, preferred_element_type=jnp.float32).astype(jnp.bfloat16)
    value_matrix = jnp.dot(normed, value_weight, preferred_element_type=jnp.float32).astype(jnp.bfloat16)
    query_groups = QUERY_HEADS // KEY_VALUE_HEADS
    query4_grouped = query_matrix.reshape(every_row, KEY_VALUE_HEADS, query_groups, HEAD_WIDTH)
    padded_keys = jnp.pad(key.reshape(every_row, KEY_VALUE_HEADS, HEAD_WIDTH), ((WINDOW_REACH, WINDOW_REACH), (0, 0), (0, 0)))
    padded_values = jnp.pad(value_matrix.reshape(every_row, KEY_VALUE_HEADS, HEAD_WIDTH), ((WINDOW_REACH, WINDOW_REACH), (0, 0), (0, 0)))
    block = TOK_DEV
    sink_column = head_sink_logit.reshape(KEY_VALUE_HEADS, query_groups, 1)

    def attend(index):
        first = (index * block).astype(jnp.int32)
        qblock = lax.dynamic_slice_in_dim(query4_grouped, first, block, 0).astype(jnp.float32)
        kblock = lax.dynamic_slice_in_dim(padded_keys, first, block + 2 * WINDOW_REACH, 0).astype(jnp.float32)
        vblock = lax.dynamic_slice_in_dim(padded_values, first, block + 2 * WINDOW_REACH, 0).astype(jnp.float32)
        scores = jnp.einsum('qkgd,jkd->kgqj', qblock, kblock) * HEAD_WIDTH ** (-0.5)
        qpos = first + jnp.arange(block, dtype=jnp.int32)
        kpos = first - WINDOW_REACH + jnp.arange(block + 2 * WINDOW_REACH, dtype=jnp.int32)
        valid = (jnp.abs(qpos[:, None] - kpos[None, :]) <= WINDOW_REACH) & (kpos[None, :] >= 0) & (kpos[None, :] < every_row)
        masked = jnp.where(valid, scores, -1e+30)
        top = jnp.maximum(lax.optimization_barrier(jnp.max(masked, axis=-1)), sink_column)
        expd = jnp.where(valid, jnp.exp(masked - top[..., None]), 0.0)
        total = lax.optimization_barrier(jnp.sum(expd, axis=-1)) + jnp.exp(sink_column - top)
        probs = (expd / total[..., None]).astype(jnp.bfloat16)
        attended = jnp.einsum('kgqj,jkd->qkgd', probs.astype(jnp.float32), vblock).astype(jnp.bfloat16)
        log_block = (top + jnp.log(total)).reshape(QUERY_HEADS, block).T
        return (attended.reshape(block, QUERY_HEADS * HEAD_WIDTH), log_block)
    attended, log_total = lax.map(attend, jnp.arange(every_row // block, dtype=jnp.int32))
    attended = attended.reshape(every_row, QUERY_HEADS * HEAD_WIDTH)
    log_total = log_total.reshape(every_row, QUERY_HEADS)
    features = jnp.concatenate([conv_out, attended], axis=1)
    weights_all = jnp.concatenate([w_out_conv, w_out_attn], axis=0)
    mixed = jnp.dot(features, weights_all, preferred_element_type=jnp.float32).astype(jnp.bfloat16)
    return (mixed, log_total)
```

```python
import functools

import jax
import jax.numpy as jnp
from jax import lax
from jax.experimental import pallas as pl
from jax.experimental.pallas import tpu as pltpu
from jax.sharding import PartitionSpec as P

WINDOW_REACH = 128


def with_halo(cells, sides, width):
    for axis, dim in sides:
        count = lax.axis_size(axis)
        ends = count - 1
        head = lax.slice_in_dim(cells, 0, width, axis=dim)
        tail = lax.slice_in_dim(cells, cells.shape[dim] - width, cells.shape[dim], axis=dim)
        cells = jnp.concatenate(
            [
                lax.ppermute(tail, axis, [(i, (i + 1) % count) for i in range(ends)]),
                cells,
                lax.ppermute(head, axis, [((i + 1) % count, i) for i in range(ends)]),
            ],
            axis=dim,
        )
    return cells


def on_device(
    tokens,
    in_gain,
    w_conv_val,
    w_conv_gate,
    w_query,
    w_key,
    value_weight,
    conv_taps,
    conv_bias,
    norm_gain,
    norm_bias,
    head_sink_logit,
    w_out_conv,
    w_out_attn,
):
    flt = tokens.astype(jnp.float32)
    normed = (
        flt * lax.rsqrt(jnp.mean(flt * flt, axis=-1, keepdims=True) + 1e-06) * in_gain
    ).astype(jnp.bfloat16)
    val_full, gate_full, query_full, key_full, value_full = (
        lax.all_gather(w_conv_val, "sp", axis=0, tiled=True),
        lax.all_gather(w_conv_gate, "sp", axis=0, tiled=True),
        lax.all_gather(w_query, "sp", axis=0, tiled=True),
        lax.all_gather(w_key, "sp", axis=0, tiled=True),
        lax.all_gather(value_weight, "sp", axis=0, tiled=True),
    )
    joined = jnp.concatenate([val_full, gate_full, query_full, key_full, value_full], axis=1)
    projected = jnp.dot(
        lax.all_gather(normed, "tp", axis=0, tiled=True), joined, preferred_element_type=jnp.float32
    )
    chans = val_full.shape[1]
    qwidth = query_full.shape[1]
    kwidth = key_full.shape[1]
    length = projected.shape[0]
    glu = (projected[:, :chans] * jax.nn.sigmoid(projected[:, chans : 2 * chans])).astype(
        jnp.bfloat16
    )
    base = 2 * chans
    query_matrix = projected[:, base : base + qwidth].astype(jnp.bfloat16)
    key = projected[:, base + qwidth : base + qwidth + kwidth].astype(jnp.bfloat16)
    value_matrix = projected[:, base + qwidth + kwidth :].astype(jnp.bfloat16)
    taps = conv_taps.shape[0]
    half = taps // 2
    padded = with_halo(glu, (("sp", 0),), half)
    filtered = jnp.zeros(glu.shape, jnp.float32) + conv_bias
    for offset in range(taps):
        filtered = (
            filtered + padded[offset : offset + length].astype(jnp.float32) * conv_taps[offset]
        )
    sums, squares = lax.psum(
        (jnp.sum(filtered, axis=-1), jnp.sum(filtered * filtered, axis=-1)), "tp"
    )
    count = chans * lax.axis_size("tp")
    center = (sums / count)[:, None]
    spread = (squares / count)[:, None] - center * center
    conv_out = jax.nn.silu(
        (filtered - center) * lax.rsqrt(spread + 1e-05) * norm_gain + norm_bias
    ).astype(jnp.bfloat16)
    heads_here = head_sink_logit.shape[0]
    head_size = qwidth // heads_here
    kv_here = kwidth // head_size
    query_groups = heads_here // kv_here
    stacked = jnp.stack([key, value_matrix], axis=0)
    banded = with_halo(stacked, (("sp", 1),), WINDOW_REACH)
    span = length + 2 * WINDOW_REACH
    key_band = banded[0].reshape(span, kv_here, head_size)
    value_band = banded[1].reshape(span, kv_here, head_size)
    query4_grouped = query_matrix.reshape(length, kv_here, query_groups, head_size)
    scores = jnp.einsum(
        "qkgd,jkd->kgqj", query4_grouped, key_band, preferred_element_type=jnp.float32
    ) * head_size ** (-0.5)
    offset_pos = lax.axis_index("sp") * length
    seq_len = length * lax.axis_size("sp")
    qpos = offset_pos + jnp.arange(length, dtype=jnp.int32)
    kpos = offset_pos - WINDOW_REACH + jnp.arange(span, dtype=jnp.int32)
    valid = (
        (jnp.abs(qpos[:, None] - kpos[None, :]) <= WINDOW_REACH)
        & (kpos[None, :] >= 0)
        & (kpos[None, :] < seq_len)
    )
    sink_column = head_sink_logit.reshape(kv_here, query_groups, 1)
    masked = jnp.where(valid, scores, -1e30)
    top = jnp.maximum(jnp.max(masked, axis=-1), sink_column)
    expd = jnp.where(valid, jnp.exp(masked - top[..., None]), 0.0)
    total = jnp.sum(expd, axis=-1) + jnp.exp(sink_column - top)
    probs = (expd / total[..., None]).astype(jnp.bfloat16)
    attended = jnp.einsum(
        "kgqj,jkd->qkgd", probs, value_band, preferred_element_type=jnp.float32
    ).astype(jnp.bfloat16)
    attended = attended.reshape(length, qwidth)
    log_total = (top + jnp.log(total)).reshape(heads_here, length).T
    out_conv_cols, out_attn_cols = (
        lax.all_gather(w_out_conv, "sp", axis=1, tiled=True),
        lax.all_gather(w_out_attn, "sp", axis=1, tiled=True),
    )
    out_rows = jnp.concatenate([out_conv_cols, out_attn_cols], axis=0)
    features = jnp.concatenate([conv_out, attended], axis=1)
    mixed = lax.psum_scatter(
        jnp.dot(features, out_rows, preferred_element_type=jnp.float32).astype(jnp.bfloat16),
        "tp",
        scatter_dimension=0,
        tiled=True,
    )
    return (mixed, log_total)


BF = jnp.bfloat16
F32 = jnp.float32


def fused_kernel(
    n, x_hbm, gain_in, wval, wgate, wquery, wkey, wvalue, taps_in, cbias_in, ngain_in, nbias_in,
    sink_in, woc, woa,
    mixed, logt,
    tok, gain, nrm, wc, wq, wo, stc, stq, sto, taps, cbias, ngain, nbias, sink,
    accq, qb, band, keven, kodd, veven, vodd, glu, filt, stat, feat, fe, lgb, lgr, ys, yr, mix,
    lsem, psem, prec, wsem, wrec, vsem, vrec, zsem, zrec, dsem, drec, xsem, xrec, esem, erec, tsem, trec, fsem,
    hsem, hrec, ssem, srec, csem, crec, ysem, yrec, gsem, grec, osem,
):
    sp = lax.axis_index("sp")
    t = lax.axis_index("tp")
    nz = n // 2
    z, x = sp // 2, sp % 2
    y, c = t // 2, t % 2
    sl, tq, slp = 2 * z + c, 2 * y + x, 2 * z + 1 - c
    same, cross = x == c, x != c
    d = (x - c) * (x - c)
    tl, width = x_hbm.shape
    length = 4 * tl
    kb, chans = wval.shape
    qwidth = wquery.shape[1]
    hd = wkey.shape[0]
    kvw = 2 * hd
    heads = sink_in.shape[1]
    ob = woc.shape[1]
    reach = WINDOW_REACH

    def dev(zz, xx, yy, cc):
        return {"sp": 2 * zz + xx, "tp": 2 * yy + cc}

    def rows(o, size):
        return pl.ds(pl.multiple_of(o * size, size), size)

    partner = dev(z, x, y, 1 - c)
    mirror = dev(z, 1 - x, y, 1 - c)
    up, down = dev(z + 1, x, y, c), dev(z - 1, x, y, c)
    has_up, has_down = z < nz - 1, z > 0

    barrier = pltpu.get_barrier_semaphore()

    def hello(to):
        pl.semaphore_signal(barrier, inc=1, device_id=to, device_id_type=pl.DeviceIdType.MESH)

    for e in range(1, 8):
        hello(dev(z, (x + e) % 2, (y + e // 2) % 2, (c + e // 4) % 2))

    @pl.when(has_up)
    def _():
        hello(up)
        hello(dev(z + 1, x, y, 1 - c))

    @pl.when(has_down)
    def _():
        hello(down)
        hello(dev(z - 1, x, y, 1 - c))

    greeted = 7 + 2 * jnp.minimum(nz - 1 - z, 1) + 2 * jnp.minimum(z, 1)

    def when(cond, fn):
        if cond is None:
            fn()
        else:
            pl.when(cond)(fn)

    def local(cond, src, dst, k):
        def make():
            return pltpu.make_async_copy(src, dst, lsem.at[k])

        when(cond, lambda: make().start())
        return lambda: make().wait()

    load_tok = local(None, x_hbm, tok, 0)
    load_gain = local(None, gain_in, gain, 1)
    params = (
        (taps_in, taps), (cbias_in, cbias), (ngain_in, ngain), (nbias_in, nbias), (sink_in, sink)
    )
    load_params = [local(same, src, dst, 2 + i) for i, (src, dst) in enumerate(params)]
    cols = rows(sp, kb)
    per_kind = (
        (
            (wval, wc.at[cols, pl.ds(0, chans)], stc.at[:, pl.ds(0, chans)]),
            (wgate, wc.at[cols, pl.ds(chans, chans)], stc.at[:, pl.ds(chans, chans)]),
        ),
        (
            (wquery, wq.at[sp, pl.ds(0, kb)], stq.at[pl.ds(0, kb)]),
            (wkey, wq.at[sp, pl.ds(kb, hd)], stq.at[pl.ds(kb, hd)]),
            (wvalue, wq.at[sp, pl.ds(kb + hd, hd)], stq.at[pl.ds(kb + hd, hd)]),
        ),
        (
            (woc, wo.at[sp, y, pl.ds(0, chans)], sto.at[pl.ds(0, chans)]),
            (woa, wo.at[sp, y, pl.ds(chans, qwidth)], sto.at[pl.ds(chans, qwidth)]),
        ),
    )
    loaded = []
    k = 7
    for group in per_kind:
        waits = []
        for src, here, there in group:
            waits.append((local(same, src, here, k), local(cross, src, there, k)))
            k += 1
        loaded.append(waits)

    def wait_loaded(kind, which):
        for pair in loaded[kind]:
            pair[which]()

    ends = []

    def remote(spec, cond=None, go=None):
        def make():
            src, dst, ss, rs, to = spec()
            return pltpu.make_async_remote_copy(
                src_ref=src, dst_ref=dst, send_sem=ss, recv_sem=rs, device_id=to,
                device_id_type=pl.DeviceIdType.MESH,
            )

        when(go() if go else None, lambda: make().start())
        ends.append((cond or go, make))

    def arrived(ref, rs, ss):
        pltpu.make_async_remote_copy(
            src_ref=ref, dst_ref=ref, send_sem=ss, recv_sem=rs, device_id=partner,
            device_id_type=pl.DeviceIdType.MESH,
        ).wait_recv()

    qdepth = (kb + kvw) // 2
    cdepth = kb // 2

    def block(k, o, h):
        if k == 0:
            return wc.at[pl.ds(pl.multiple_of(o * kb + h * cdepth, cdepth), cdepth)]
        if k == 1:
            return wq.at[o, pl.ds(pl.multiple_of(h * qdepth, 64), qdepth)]
        return wo.at[o, y, rows(h, chans)]

    def carried(k, zs, e, core):
        return block(k, 2 * zs + (x if e == 0 else 1 - x), core)

    def staged(k, h):
        if k == 0:
            return stc.at[pl.ds(h * cdepth, cdepth)]
        if k == 1:
            return stq.at[pl.ds(h * qdepth, qdepth)]
        return sto.at[pl.ds(h * chans, chans)]

    def hop(k, e, zs, way, cond, go):
        def spec():
            ref = carried(k, zs, e, c)
            to = up if way == 0 else down
            return ref, ref, zsem.at[k, e, zs, way], zrec.at[k, e, zs], to

        remote(spec, cond, go)

    def share(k, e, zs, cond):
        def spec():
            ref = carried(k, zs, e, c)
            return ref, ref, dsem.at[k, e, zs], drec.at[k, e, zs], partner

        remote(spec, cond)

    def across_y(e, zs, cond):
        def spec():
            ref = carried(2, zs, e, c)
            return ref, ref, xsem.at[e, zs], xrec.at[e, zs], dev(z, x, 1 - y, c)

        remote(spec, cond)

    def far_half(e, zs, core):
        return wo.at[2 * zs + (x if e == 0 else 1 - x), 1 - y, rows(core, chans)]

    def from_y(e, zs):
        ref = far_half(e, zs, c)
        arrived(ref, xrec.at[e, zs], xsem.at[e, zs])
        remote(lambda: (ref, ref, esem.at[e, zs], erec.at[e, zs], partner))

    def from_y_shared(e, zs):
        arrived(far_half(e, zs, 1 - c), erec.at[e, zs], esem.at[e, zs])

    mid = has_up & has_down
    low, high = z < nz // 2, z >= nz // 2
    hi = z // 2
    zorder = (z, 4 * hi + 1 - z, 2 - hi, 3 - 3 * hi)

    def flow(k, s, es=(0, 1), only=None, pass_on=True, inner=False):
        below, above = z - s, z + s

        def valid(zs, side):
            ok = (zs >= 0) & (zs <= nz - 1) & side
            return ok & only() if only else ok

        def land(e, zs, way, cond, more, closer):
            arrived(carried(k, zs, e, c), zrec.at[k, e, zs], zsem.at[k, e, zs, way])
            if s < nz - 1 and pass_on:
                hop(k, e, zs, way, lambda: cond() & more, lambda: more)
            if k == 2 and inner:

                @pl.when(closer)
                def _():
                    across_y(e, zs, lambda: cond() & closer)
            elif k == 2:
                across_y(e, zs, cond)
            share(k, e, zs, cond)

        for zs, way, more, closer, side in (
            (above, 1, has_down, low, low),
            (below, 0, has_up, high, low | high),
            (above, 1, has_down, low, high),
        ):
            for e in es:

                @pl.when(valid(zs, side))
                def _():
                    land(
                        e, zs, way, lambda zs=zs, side=side: valid(zs, side), more, closer
                    )

    def shared(k, e, zs):
        arrived(carried(k, zs, e, 1 - c), drec.at[k, e, zs], dsem.at[k, e, zs])

    def all_shared(k, p):
        if p == 0:

            @pl.when(cross)
            def _():
                shared(k, 0, z)
        else:
            shared(k, 0, zorder[p])
        shared(k, 1, zorder[p])

    def swap(k):
        @pl.when(cross)
        def _():
            wait_loaded(k, 1)
            for h in (0, 1):
                remote(
                    lambda h=h: (
                        staged(k, h), block(k, sp, h), wsem.at[k, h], wrec.at[k],
                        dev(z, 1 - x, y, h),
                    ),
                    lambda: cross,
                )

    def give(k):
        @pl.when(same)
        def _():
            wait_loaded(k, 0)
            remote(
                lambda: (
                    block(k, sp, 1 - c), block(k, sp, 1 - c), vsem.at[k], vrec.at[k], partner
                ),
                lambda: same,
            )
            if k < 2:
                hop(k, 0, z, 0, lambda: same & has_up, lambda: has_up)
                hop(k, 0, z, 1, lambda: same & has_down, lambda: has_down)
            share(k, 0, z, lambda: same)

    def given(k):
        @pl.when(cross)
        def _():
            arrived(carried(k, z, 0, c), vrec.at[k], vsem.at[k])
            if k < 2:
                hop(k, 0, z, 0, lambda: cross & has_up, lambda: has_up)
                hop(k, 0, z, 1, lambda: cross & has_down, lambda: has_down)

    def swapped(k):
        arrived(carried(k, z, 1, c), wrec.at[k], wsem.at[k, 0])
        if k < 2:
            hop(k, 1, z, 0, None, lambda: has_up)
            hop(k, 1, z, 1, None, lambda: has_down)
        share(k, 1, z, None)

    jown = 2 * y + c
    across = dev(z, 1 - x, y, x)
    jslot = (1 - d) * jown + 4 * d
    hl = tl // 2

    def half_block(j, h):
        return nrm.at[pl.ds(pl.multiple_of(j * tl + h * hl, hl), hl)]

    def tok_send(e, to, h, cond=None, go=None):
        remote(
            lambda: (
                half_block(jslot, h), half_block(jown, h), tsem.at[e, h], trec.at[jown, h], to
            ),
            cond, go,
        )

    def tok_wait(j, h):
        arrived(half_block(j, h), trec.at[j, h], fsem.at[h])

    load_tok()
    load_gain()
    step = 32

    def norm_body(i, carry):
        r = pl.ds(pl.multiple_of(i * step, step), step)
        flt = tok[r, :].astype(F32)
        scale = lax.rsqrt(jnp.mean(flt * flt, axis=-1, keepdims=True) + 1e-06)
        w = pl.ds(pl.multiple_of(jslot * tl + i * step, step), step)
        nrm[w, :] = (flt * scale * gain[...]).astype(BF)
        return carry

    lax.fori_loop(0, tl // step, norm_body, 0)
    pl.semaphore_wait(barrier, greeted)

    swap(0)
    give(0)
    give(1)
    for h in (0, 1):
        tok_send(0, dev(z, x, 1 - y, x), h)
    for h in (0, 1):
        tok_send(2, partner, h, None, lambda: cross)
    @pl.when(same)
    def _():
        for i, (src, dst) in enumerate(params):
            load_params[i]()
            remote(
                lambda i=i, dst=dst: (dst, dst, psem.at[i], prec.at[i], partner), lambda: same
            )

    @pl.when(cross)
    def _():
        for h in (0, 1):
            tok_send(1, across, h, lambda: cross)

    given(0)
    given(1)
    swapped(0)

    @pl.when(same)
    def _():
        for h in (0, 1):
            tok_send(1, across, h, lambda: same)

    flow(0, 1)
    swap(1)
    jfwd = (1 - d) * (2 * (1 - y) + 1) + d * 2 * y
    fwd_dev = {
        "sp": (1 - d) * (2 * z + 1 - x) + d * sp,
        "tp": (1 - d) * (2 * y + c) + d * (2 * (1 - y) + c),
    }

    def tok_forward(h):
        tok_wait(jfwd, h)
        remote(
            lambda: (
                half_block(jfwd, h), half_block(jfwd, h), fsem.at[h], trec.at[jfwd, h], fwd_dev
            )
        )

    tok_forward(0)
    flow(0, 2)

    tok_forward(1)
    swapped(1)
    swap(2)
    give(2)
    flow(0, 3)
    given(2)
    across_y(0, z, None)

    pad = 16

    def project_conv(yy):
        at = pl.ds(pl.multiple_of(yy * 2 * tl, 2 * tl), 2 * tl)
        res = jnp.dot(nrm[at, :], wc[...], preferred_element_type=F32)
        glu[pl.ds(pl.multiple_of(pad + yy * 2 * tl, pad), 2 * tl), :] = (
            (res[:, 0:chans] * jax.nn.sigmoid(res[:, chans : 2 * chans])).astype(BF).astype(F32)
        )

    for h in (0, 1):
        tok_wait((1 - d) * (2 * y + 1 - c) + d * (2 * y + 1), h)
    for p in range(nz):
        all_shared(0, p)
    def at_mid():
        return mid

    def at_end():
        return jnp.logical_not(mid)

    project_conv(y)
    flow(1, 1, only=at_mid)
    for h in (0, 1):
        tok_wait(2 * (1 - y), h)

    @pl.when(cross)
    def _():
        for h in (0, 1):
            tok_wait(2 * (1 - y) + 1, h)
        for i, (src, dst) in enumerate(params):
            arrived(dst, prec.at[i], psem.at[i])

    project_conv(1 - y)
    zn, zp = jnp.minimum(z + c, nz - 1), jnp.maximum(z - 1 + c, 0)
    nxt, prv = dev(zn, x, y, 1 - c), dev(zp, x, y, 1 - c)
    has_nxt, has_prv = sl < n - 1, sl > 0

    def halo(buf, size, base):
        remote(
            lambda: (
                buf.at[pl.ds(length, size)], buf.at[pl.ds(0, size)], hsem.at[base],
                hrec.at[base], nxt,
            ),
            None, lambda: has_nxt,
        )
        remote(
            lambda: (
                buf.at[pl.ds(size, size)], buf.at[pl.ds(length + size, size)], hsem.at[base + 1],
                hrec.at[base + 1], prv,
            ),
            None, lambda: has_prv,
        )

    def halo_wait(buf, size, base):
        @pl.when(has_prv)
        def _():
            arrived(buf.at[pl.ds(0, size)], hrec.at[base], hsem.at[base])

        @pl.when(has_nxt)
        def _():
            arrived(buf.at[pl.ds(length + size, size)], hrec.at[base + 1], hsem.at[base + 1])

        @pl.when(sl == 0)
        def _():
            buf[pl.ds(0, size), :] = jnp.zeros((size, buf.shape[1]), buf.dtype)

        @pl.when(sl == n - 1)
        def _():
            buf[pl.ds(length + size, size), :] = jnp.zeros((size, buf.shape[1]), buf.dtype)

    halo(glu, pad, 0)
    swapped(2)
    across_y(1, z, None)
    for e in (0, 1):
        hop(2, e, z, 0, None, lambda: low)
        hop(2, e, z, 1, None, lambda: high)
    ntaps = taps.shape[0]
    off = pad - ntaps // 2
    cstep = 64

    def conv_rows(r0):
        acc = jnp.zeros((cstep, chans), F32) + cbias[...]
        for j in range(ntaps):
            acc = acc + glu[pl.ds(r0 + off + j, cstep), :] * taps[pl.ds(j, 1), :]
        filt[pl.ds(r0, cstep), :] = acc

    nconv = length // cstep
    for i in range(1, nconv // 2):
        conv_rows(i * cstep)
    flow(1, 2, only=at_mid)
    for i in range(nconv // 2, nconv - 1):
        conv_rows(i * cstep)
    flow(1, 1, only=at_end)
    halo_wait(glu, pad, 0)
    conv_rows(0)
    conv_rows((nconv - 1) * cstep)
    lane = lax.broadcasted_iota(jnp.int32, (128, 128), 1)
    for b in range(length // 128):
        f = filt[pl.ds(b * 128, 128), :]
        s1 = jnp.sum(f, axis=-1, keepdims=True)
        s2 = jnp.sum(f * f, axis=-1, keepdims=True)
        tile = jnp.where(lane == 0, s1, jnp.where(lane == 1, s2, 0.0))
        stat[pl.ds(tq, 1), :, pl.ds(b * 128, 128)] = jnp.transpose(tile)[None, 0:8, :]
    peers = ((x, 1 - y), (1 - x, 1 - y), (1 - x, y))
    for e, (px, py) in enumerate(peers):
        remote(
            lambda e=e, px=px, py=py: (
                stat.at[tq], stat.at[tq], ssem.at[e], srec.at[tq], dev(z, px, py, c)
            )
        )
    def project_heads(p):
        all_shared(1, p)
        kv, qs = 0.0, 0.0
        for e in (0, 1):
            o = 2 * zorder[p] + e
            lhs = nrm[0:length, rows(o, kb)]
            kv = kv + lax.dot_general(
                lhs, wq[o, kb : kb + kvw, :], (((1,), (1,)), ((), ())), preferred_element_type=F32
            )
            qs = qs + jnp.dot(lhs, wq[o, 0:kb, :], preferred_element_type=F32)
        if p > 0:
            kv = kv + accq[:, qwidth : qwidth + kvw]
            qs = qs + accq[:, 0:qwidth]
        if p < nz - 1:
            accq[:, qwidth : qwidth + kvw] = kv
            accq[:, 0:qwidth] = qs
        else:
            band[pl.ds(reach, length), :] = kv.astype(BF)
            qb[...] = (qs * hd ** (-0.5)).astype(BF)

    for h in (0, 1):
        hop(2, h, z, 0, None, lambda: mid & high)
        hop(2, h, z, 1, None, lambda: mid & low)
    flow(1, 2, only=at_end)
    project_heads(0)
    project_heads(1)
    flow(2, 1, only=at_mid, pass_on=False, inner=True)
    for px, py in peers:
        arrived(stat.at[2 * py + px], srec.at[2 * py + px], ssem.at[0])
    count = chans * 4
    for b in range(length // 128):
        at = pl.ds(b * 128, 128)
        tot = (stat[0, :, at] + stat[1, :, at] + stat[2, :, at] + stat[3, :, at]) / count
        tt = jnp.transpose(jnp.concatenate([tot] * 16, axis=0))
        center = tt[:, 0:1]
        spread = tt[:, 1:2] - center * center
        u = (filt[at, :] - center) * lax.rsqrt(spread + 1e-05)
        u = u * ngain[...] + nbias[...]
        feat[at, 0:chans] = (u * jax.nn.sigmoid(u)).astype(BF)

    def place(j, kind):
        js, cs = j // 2, j % 2
        here = (cs == c) & (js == y)
        away = jnp.logical_not(here)
        r, q = rows(j, tl), pl.ds(kind * chans, chans)
        r2 = rows(c, tl)
        q2 = pl.ds(pl.multiple_of(y * (chans + qwidth) + kind * chans, chans), chans)

        @pl.when(here)
        def _():
            fe[r2, q2] = feat[r, q]

        remote(
            lambda: (
                feat.at[r, q], fe.at[r2, q2], csem.at[kind, j], crec.at[y, kind, c],
                dev(z, x, js, cs),
            ),
            None, lambda: away,
        )

    for j in range(4):
        place(j, 0)
    project_heads(2)
    flow(1, 3)
    project_heads(3)
    halo(band, reach, 2)
    for h in (0, 1):
        hop(2, h, z + 1, 1, None, at_mid)
        hop(2, h, z - 1, 0, None, at_mid)
        from_y(h, z)

    def spread_heads(r0, size):
        at = pl.ds(r0, size)
        b = band[at, :].astype(F32)
        swapped = jnp.concatenate([b[:, hd:], b[:, :hd]], axis=1)
        low = lax.broadcasted_iota(jnp.int32, (size, kvw), 1) < hd
        keven[at, :] = jnp.where(low, b, 0.0).astype(BF)
        vodd[at, :] = jnp.where(low, 0.0, b).astype(BF)
        veven[at, :] = jnp.where(low, swapped, 0.0).astype(BF)
        kodd[at, :] = jnp.where(low, 0.0, swapped).astype(BF)

    spread_heads(reach, length)
    nblk = length // reach
    ri = lax.broadcasted_iota(jnp.int32, (reach, reach), 0)
    ci = lax.broadcasted_iota(jnp.int32, (reach, reach), 1)
    log2e = 1.4426950408889634

    def attend(b):
        span = pl.ds(pl.multiple_of(b * reach, reach), 3 * reach)
        at = rows(b, reach)
        first = reach * (1 - jnp.minimum(sl, 1)) * (1 - jnp.minimum(b, 1))
        last = reach * (1 - jnp.minimum(n - 1 - sl, 1)) * (1 - jnp.minimum(nblk - 1 - b, 1))
        keep_l = ci >= ri + first
        keep_r = ci + last <= ri
        logs = []
        for pair in range(heads // 2):
            q2 = qb[at, pair * kvw : (pair + 1) * kvw]
            acc, inv = None, []
            for e, (kk, vv) in enumerate(((keven, veven), (kodd, vodd))):
                s = lax.dot_general(
                    q2, kk[span, :], (((1,), (1,)), ((), ())), preferred_element_type=F32
                )
                sa = jnp.where(keep_l, s[:, 0:reach], -1e30)
                sb = s[:, reach : 2 * reach]
                sc = jnp.where(keep_r, s[:, 2 * reach :], -1e30)
                h = 2 * pair + e
                sk = sink[0:1, h : h + 1]
                top = jnp.maximum(
                    jnp.max(jnp.maximum(jnp.maximum(sa, sb), sc), axis=-1, keepdims=True), sk
                )
                ea = jnp.exp2((sa - top) * log2e)
                eb = jnp.exp2((sb - top) * log2e)
                ec = jnp.exp2((sc - top) * log2e)
                total = jnp.sum(ea + eb + ec, axis=-1, keepdims=True) + jnp.exp(sk - top)
                p = jnp.concatenate([ea.astype(BF), eb.astype(BF), ec.astype(BF)], axis=1)
                a = jnp.dot(p, vv[span, :], preferred_element_type=F32)
                acc = a if acc is None else acc + a
                inv.append(1.0 / total)
                logs.append(top + jnp.log(total))
            acc = acc * jnp.where(lane < hd, inv[0], inv[1])
            feat[at, chans + pair * kvw : chans + (pair + 1) * kvw] = acc.astype(BF)
        wide = jnp.zeros((reach, 128), F32)
        for h in range(heads):
            wide = jnp.where(lane == h, logs[h], wide)
        lgb[:, at] = jnp.transpose(wide)[0:heads, :]

    far, near = 1 - x, x
    for b in range(1, nblk - 1):
        attend(b)
        place(b, 1)
    halo_wait(band, reach, 2)
    spread_heads(0, reach)
    spread_heads(length + reach, reach)
    flow(2, 1, (0,), at_end)
    attend(0)
    place(0, 1)
    flow(2, 1, (1,), at_end)
    attend(nblk - 1)
    place(nblk - 1, 1)
    outer_z = z - 1 + 2 * hi
    for e in (0, 1):

        def late(e=e):
            ref = carried(2, outer_z, e, c)
            return ref, ref, xsem.at[e, outer_z], xrec.at[e, outer_z], dev(z, x, 1 - y, c)

        remote(late, None, at_mid)

    @pl.when(cross)
    def _():
        remote(lambda: (lgb, lgr, gsem.at[0], grec.at[0], mirror), lambda: cross)

    def gathered(xs):
        for kind in (0, 1):
            for yy, cond in ((y, xs != c), (1 - y, None)):

                def wait(yy=yy, kind=kind):
                    q2 = pl.ds(
                        pl.multiple_of(yy * (chans + qwidth) + kind * chans, chans), chans
                    )
                    arrived(fe.at[rows(xs, tl), q2], crec.at[yy, kind, xs], csem.at[kind, 0])

                when(cond, wait)

    depth = chans + qwidth

    def half_product(js, o):
        lhs = fe[rows(js, tl), :]
        return jnp.dot(lhs[:, 0:depth], wo[o, 0], preferred_element_type=F32) + jnp.dot(
            lhs[:, depth:], wo[o, 1], preferred_element_type=F32
        )

    def column(p, par):
        return 2 * zorder[p] + par

    def emit(p, e):
        par = x if e == 0 else 1 - x
        i = 2 * p + par
        ys[i] = half_product(far, column(p, par)).astype(BF)
        remote(
            lambda: (ys.at[i], yr.at[i], ysem.at[i], yrec.at[i], dev(z, 1 - x, y, c))
        )

    def written(p, par):
        at = rows(column(p, par), ob)
        return pltpu.make_async_copy(mix.at[:, at], mixed.at[:, at], osem.at[2 * p + par])

    def finish(p, e):
        par = 1 - x if e == 0 else x
        i = 2 * p + par
        part = half_product(near, column(p, par))
        arrived(yr.at[i], yrec.at[i], ysem.at[i])
        mix[:, rows(column(p, par), ob)] = (part + yr[i].astype(F32)).astype(BF)
        written(p, par).start()

    flow(2, 2, only=at_mid)
    gathered(far)
    all_shared(2, 0)
    for e in (0, 1):
        from_y_shared(e, z)
        emit(0, e)
    gathered(near)
    steps = [(p, e) for p in range(1, nz) for e in (0, 1)]
    emitted = [(0, 0), (0, 1)]
    done = 0

    def settle(p, e):
        shared(2, e, zorder[p])
        from_y_shared(e, zorder[p])
        emit(p, e)
        emitted.append((p, e))

    for k, (p, e) in enumerate(steps):
        if p < nz - 1:
            flow(2, p + 1, (e,), at_end)
        from_y(e, zorder[p])
        if k > 0:
            settle(*steps[k - 1])
        if len(emitted) - done > 3:
            finish(*emitted[done])
            done += 1
    settle(*steps[-1])
    for u in emitted[done:]:
        finish(*u)

    @pl.when(same)
    def _():
        logt[...] = lgb[...]

    @pl.when(cross)
    def _():
        arrived(lgr, grec.at[0], gsem.at[0])
        logt[...] = lgr[...]

    for p in range(nz):
        for par in (0, 1):
            written(p, par).wait()
    for cond, make in ends:
        when(cond() if cond else None, lambda make=make: make().wait_send())


def layer(
    n, parts, tokens, in_gain, w_conv_val, w_conv_gate, w_query, w_key, value_weight, conv_taps,
    conv_bias, norm_gain, norm_bias, head_sink_logit, w_out_conv, w_out_attn,
):
    tl, width = tokens.shape
    kb, chans = w_conv_val.shape
    qwidth = w_query.shape[1]
    kvw = 2 * w_key.shape[1]
    heads = head_sink_logit.shape[0]
    ob = w_out_conv.shape[1]
    fits = (
        parts == 4 and n == 8 and tl % 128 == 0 and kb % 128 == 0 and ob % 128 == 0 and n * ob == width and chans == qwidth
        and chans % 128 == 0 and kvw == 128 and kb == qwidth and qwidth == heads * kvw // 2
        and conv_taps.shape[0] <= 33 and heads % 2 == 0
    )
    if not fits:
        return on_device(
            tokens, in_gain, w_conv_val, w_conv_gate, w_query, w_key, value_weight, conv_taps,
            conv_bias, norm_gain, norm_bias, head_sink_logit, w_out_conv, w_out_attn,
        )
    length = 4 * tl
    nz = n // 2
    vm = pl.BlockSpec(memory_space=pltpu.VMEM)
    hb = pl.BlockSpec(memory_space=pl.ANY)
    dma = pltpu.SemaphoreType.DMA
    mixed, log_rows = pl.pallas_call(
        functools.partial(fused_kernel, n),
        out_shape=(
            jax.ShapeDtypeStruct((tl, width), BF),
            jax.ShapeDtypeStruct((heads, length), F32),
        ),
        in_specs=[hb] * 14,
        out_specs=(hb, vm),
        scratch_shapes=[
            pltpu.VMEM((tl, width), BF),
            pltpu.VMEM((1, width), F32),
            pltpu.VMEM((5 * tl, width), BF),
            pltpu.VMEM((n * kb, 2 * chans), BF),
            pltpu.VMEM((n, kb + kvw, qwidth), BF),
            pltpu.VMEM((n, 2, chans + qwidth, ob), BF),
            pltpu.VMEM((kb, 2 * chans), BF),
            pltpu.VMEM((kb + kvw, qwidth), BF),
            pltpu.VMEM((chans + qwidth, ob), BF),
            pltpu.VMEM(conv_taps.shape, F32),
            pltpu.VMEM((1, chans), F32),
            pltpu.VMEM((1, chans), F32),
            pltpu.VMEM((1, chans), F32),
            pltpu.VMEM((1, heads), F32),
            pltpu.VMEM((length, qwidth + kvw), F32),
            pltpu.VMEM((length, qwidth), BF),
            *[pltpu.VMEM((length + 2 * WINDOW_REACH, kvw), BF)] * 5,
            pltpu.VMEM((length + 32, chans), F32),
            pltpu.VMEM((length, chans), F32),
            pltpu.VMEM((4, 8, length), F32),
            pltpu.VMEM((length, chans + qwidth), BF),
            pltpu.VMEM((2 * tl, 2 * (chans + qwidth)), BF),
            pltpu.VMEM((heads, length), F32),
            pltpu.VMEM((heads, length), F32),
            pltpu.VMEM((n, tl, ob), BF),
            pltpu.VMEM((n, tl, ob), BF),
            pltpu.VMEM((tl, width), BF),
            dma((14,)),
            dma((5,)),
            dma((5,)),
            dma((3, 2)),
            dma((3,)),
            dma((3,)),
            dma((3,)),
            dma((3, 2, nz, 2)),
            dma((3, 2, nz)),
            dma((3, 2, nz)),
            dma((3, 2, nz)),
            dma((2, nz)),
            dma((2, nz)),
            dma((2, nz)),
            dma((2, nz)),
            dma((3, 2)),
            dma((4, 2)),
            dma((3,)),
            dma((4,)),
            dma((4,)),
            dma((3,)),
            dma((4,)),
            dma((2, 4)),
            dma((2, 2, 2)),
            dma((n,)),
            dma((n,)),
            dma((1,)),
            dma((1,)),
            dma((n,)),
        ],
        compiler_params=pltpu.CompilerParams(
            collective_id=0, has_side_effects=True, vmem_limit_bytes=56 * 1024 * 1024
        ),
    )(
        tokens, in_gain.reshape(1, width), w_conv_val, w_conv_gate, w_query, w_key.T, value_weight.T,
        conv_taps, conv_bias.reshape(1, chans), norm_gain.reshape(1, chans), norm_bias.reshape(1, chans),
        head_sink_logit.reshape(1, heads), w_out_conv, w_out_attn,
    )
    return mixed, log_rows.T


def solution(mesh):
    return jax.shard_map(
        functools.partial(layer, mesh.shape["sp"], mesh.shape["tp"]),
        mesh=mesh,
        in_specs=(
            P(("sp", "tp"), None),
            P(),
            P("sp", "tp"),
            P("sp", "tp"),
            P("sp", "tp"),
            P("sp", "tp"),
            P("sp", "tp"),
            P(None, "tp"),
            P("tp"),
            P("tp"),
            P("tp"),
            P("tp"),
            P("tp", "sp"),
            P("tp", "sp"),
        ),
        out_specs=(P(("sp", "tp"), None), P("sp", "tp")),
        check_vma=False,
    )
```
